32 devices in a mesh: fs: 8 (over z, y), tp: 4 (over x, core).
Axes of the slice: x: 2, y: 2, z: 4, core: 2. Of those that a mesh axis runs over, the one named last changes fastest.
Arguments:
- tokens: bfloat16 [3072, 2048], P('tp'), may hold values from -6 to 6
- norm_gain: float32 [2048], P('fs'), may hold values from 0.1 to 1.9
- gate_weight: float32 [4, 2048, 8192], P(None, 'fs', 'tp'), may hold values from -0.125 to 0.125
- up_weight: float32 [4, 2048, 8192], P(None, 'fs', 'tp'), may hold values from -0.125 to 0.125
- down_weight: float32 [4, 8192, 2048], P(None, 'fs', 'tp'), may hold values from -0.0625 to 0.0625
- routes: int32 [3072, 2], P('tp'), may hold values from 0 to 3, all different within a row; in each aligned block of 768 rows (0 to 767, 768 to 1535, ...) at most 480 rows name the same one
- route_logit: float32 [3072, 2], P('tp'), may hold values from -6 to 6
Outputs:
- gate_out: bfloat16 [4, 2048, 8192], P(None, None, 'fs')
- up_out: bfloat16 [4, 2048, 8192], P(None, None, 'fs')
- down_out: bfloat16 [4, 8192, 2048], P(None, 'fs')
- mixed: bfloat16 [3072, 2048], P(('tp', 'fs'))
The draws below stay inside these ranges and needn't reach their ends.
Inputs may be any that keep to these rules, and one draw needn't show every extreme that they name: `routes`: the two experts of a token differ. In each aligned block of 768 tokens (the tokens of one request group) every expert is named by at most 480 tokens, a bound that some block reaches.
All inputs are finite; a program needn't handle non-finite values.
Results may differ from the reference program's by a relative error of at most 0.0082.
Values may be sent and summed in bfloat16 or wider, within the bound.
A program may use at most 192 MiB of HBM per device.

```python
import math
import jax
import jax.numpy as jnp
import numpy as np
from jax import lax

D = 2048
FF = 8192
E = 4
TOK_GROUP = 768
CAP = 480
TOKENS = 3072


def levels(stream_key, dims, shards, least, largest):
    factor_of = 1.0
    for axis_at, parts in shards:
        steps = jax.random.uniform(jax.random.fold_in(jax.random.fold_in(stream_key, 6), axis_at), (parts,), jnp.float32, least / len(shards), largest / len(shards))
        factor_of = factor_of * jnp.repeat(jnp.exp(steps), dims[axis_at] // parts).reshape((-1,) + (1,) * (len(dims) - 1 - axis_at))
    return factor_of


def deal_out(rng, own, number, rows, number_of, top, limit, skew):
    sequence = jax.random.permutation(rng, number_of)
    packed, ordinary = load_shares(number_of, rows * top, limit, skew, True), load_shares(number_of, rows * top, limit, skew, False)
    places = jnp.arange(number_of)

    def named(tallies, rotation):
        used = int((tallies > 0).sum())
        fixed = max(1, used // 4)
        passed = fixed + (places - fixed + rotation * (used - fixed)) % max(1, number_of - fixed)
        return jnp.zeros((number_of,), jnp.int32).at[sequence[jnp.where(places < fixed, places, passed)]].set(jnp.asarray(tallies, jnp.int32))

    tallies = jnp.where(number % 4 == 0, named(packed, number // 4), named(ordinary, number - number // 4 - 1))
    mixed = jax.random.permutation(jax.random.fold_in(own, 3), number_of)
    source_of, receiver = mixed[0:number_of // 2 * 2:2], mixed[1:number_of // 2 * 2:2]
    margin = jnp.minimum(tallies[source_of] - 1, limit - tallies[receiver]) // 2
    margin = jnp.where((source_of == sequence[0]) | (receiver == sequence[0]) | (tallies[receiver] == 0), 0, jnp.maximum(margin, 0))
    passed = jax.random.randint(jax.random.fold_in(own, 4), (number_of // 2,), 0, 1 << 20) % (margin + 1)
    tallies = tallies.at[source_of].add(-passed).at[receiver].add(passed)
    items = jnp.searchsorted(jnp.cumsum(tallies), jnp.arange(rows * top), side="right").astype(jnp.int32)
    grid = items.reshape(top, rows).T
    grid = grid[jax.random.permutation(jax.random.fold_in(own, 1), rows)]
    rotation = jax.random.randint(jax.random.fold_in(own, 2), (rows, 1), 0, top)
    return jnp.take_along_axis(grid, (jnp.arange(top)[None, :] + rotation) % top, axis=1)


def load_shares(amount, total, bound, skew, full):
    loads = [(1 << 20) // math.isqrt(grade ** skew) + 1 for grade in range(1, amount + 1)]
    largest = bound if full else min(bound, max(-(-total // amount), total * loads[0] // sum(loads)))
    least = 1 if total - largest >= amount - 1 else 0
    counts, spare = [largest] + [least] * (amount - 1), total - largest - least * (amount - 1)
    while spare > 0:
        movable = [i for i in range(1, amount) if counts[i] < largest] or [i for i in range(1, amount) if counts[i] < bound]
        pool, left = sum([loads[i] for i in movable]), spare
        for i in movable:
            more = min(bound - counts[i], max(1, left * loads[i] // pool), spare)
            counts[i] = counts[i] + more
            spare = spare - more
    return np.array(counts)


def scatter_about(stream_key, shape, deviation, limit, pieces=(), held_as=jnp.bfloat16):
    entries = jax.random.normal(stream_key, shape, jnp.float32) * deviation
    if len(pieces) > 0:
        entries = levels(stream_key, shape, pieces, -0.22, 0.18) * entries
    return jnp.clip(entries, min=-limit, max=limit).astype(held_as)


def setup_inputs(seed: int = 0) -> dict:
    seeds = jax.random.split(jax.random.key(seed), 8)
    tokens = scatter_about(seeds[0], (TOKENS, D), 1.0, 6.0, ((0, 4),))
    norm_gain = jnp.clip(1.0 + 0.18 * jax.random.normal(seeds[1], (D,), jnp.float32), 0.1, 1.9)
    gate_weight = scatter_about(seeds[2], (E, D, FF), D ** -0.5, 0.125, ((1, 8), (2, 4)), jnp.float32)
    up_weight = scatter_about(seeds[3], (E, D, FF), D ** -0.5, 0.125, ((1, 8), (2, 4)), jnp.float32)
    down_weight = scatter_about(seeds[4], (E, FF, D), FF ** -0.5, 0.0625, ((1, 8), (2, 4)), jnp.float32)
    routes_keys = jax.random.split(jax.random.fold_in(seeds[5], 1), TOKENS // TOK_GROUP)
    routes_turns = jax.random.permutation(jax.random.fold_in(seeds[5], 3), TOKENS // TOK_GROUP)
    routes = jax.vmap(lambda own, number: deal_out(jax.random.fold_in(seeds[5], 2), own, number, TOK_GROUP, E, 2, CAP, 1))(routes_keys, routes_turns).reshape((TOKENS, 2))
    route_logit = scatter_about(seeds[6], (TOKENS, 2), 1.0, 6.0, ((0, 4),), jnp.float32)
    return dict(tokens=tokens, norm_gain=norm_gain, gate_weight=gate_weight, up_weight=up_weight, down_weight=down_weight, routes=routes, route_logit=route_logit)


EPS = 0.5

def reference(tokens, norm_gain, gate_weight, up_weight, down_weight, routes, route_logit):
    gain_col = norm_gain.astype(jnp.float32)[None, :, None]
    gate_out = (gate_weight * gain_col).astype(jnp.bfloat16)
    up_out = (up_weight * gain_col).astype(jnp.bfloat16)
    down_out = down_weight.astype(jnp.bfloat16)
    floats = tokens.astype(jnp.float32)
    normed = (floats * lax.rsqrt(lax.optimization_barrier(jnp.mean(floats * floats, axis=1, keepdims=True)) + EPS)).astype(jnp.bfloat16)
    first_share = jax.nn.sigmoid(route_logit[:, 0] - route_logit[:, 1])
    shares = jnp.stack([first_share, 1.0 - first_share], axis=1)
    summed = jnp.zeros(tokens.shape, jnp.float32)
    for expert in range(E):
        weight_col = lax.optimization_barrier(jnp.sum(jnp.where(routes == expert, shares, 0.0), axis=1, keepdims=True))
        gate_val = jnp.dot(normed, gate_out[expert], preferred_element_type=jnp.float32)
        up_val = jnp.dot(normed, up_out[expert], preferred_element_type=jnp.float32)
        hidden = (jax.nn.silu(gate_val) * up_val).astype(jnp.bfloat16)
        result = jnp.dot(hidden, down_out[expert], preferred_element_type=jnp.float32)
        summed = summed + weight_col * result
    return (gate_out, up_out, down_out, summed.astype(jnp.bfloat16))
```

```python
import functools

import jax
import jax.numpy as jnp
from jax import lax
from jax.experimental import pallas as pl
from jax.experimental.pallas import tpu as pltpu
from jax.sharding import PartitionSpec as P

EPS = 0.5
MESH = pl.DeviceIdType.MESH
VMEM_LIMIT = 62 * 1024 * 1024


def spread(
    fs_size, tp_size,
    gate, up, down,
    gate_all, up_all, down_all, gate_far, up_far,
    across_send, across_recv, near_send, near_recv, far_send, twin_send, twin_recv,
    down_send, down_recv,
):
    experts, depth, width = gate.shape
    units = gate_all.shape[2]
    per = width // units
    fs, tp = lax.axis_index("fs"), lax.axis_index("tp")
    half, side = tp // 2, tp % 2
    twin = half * 2 + 1 - side
    across = (1 - half) * 2 + side
    col = down.shape[2]

    def remote(src, dst, send, recv, fs_to, tp_to):
        return pltpu.make_async_remote_copy(
            src_ref=src, dst_ref=dst, send_sem=send, recv_sem=recv,
            device_id=(fs_to, tp_to), device_id_type=MESH,
        )

    def columns(owner):
        return pl.ds(pl.multiple_of(owner * col, col), col)

    pieces = [(a, e) for e in range(experts) for a in range(2)]
    own, far, full = (gate, up), (gate_far, up_far), (gate_all, up_all)

    crossing = []
    for a, e in pieces:
        copy = remote(
            own[a].at[e], far[a].at[e], across_send.at[a, e], across_recv.at[a, e], fs, across
        )
        copy.start()
        crossing.append(copy)

    rows = pl.ds(pl.multiple_of(fs * depth, depth), depth)

    def deal(source, a, e, owner, sem):
        for h in range(per):
            remote(
                source[a].at[e, :, pl.ds(h * units, units)],
                full[a].at[e, rows, :],
                sem.at[a, e],
                near_recv.at[a, e],
                owner * per + h,
                twin,
            ).start()

    for a, e in pieces:
        deal(own, a, e, tp, near_send)

    down_near = remote(
        down, down_all.at[:, :, columns(tp)], down_send.at[0], down_recv.at[0], fs, twin
    )
    down_near.start()
    down_far = remote(
        down, down_all.at[:, :, columns(tp)], down_send.at[1], down_recv.at[1], fs, across
    )
    down_far.start()

    for (a, e), copy in zip(pieces, crossing):
        copy.wait_recv()
        deal(far, a, e, across, far_send)

    def hand_down(owner, index):
        return remote(
            down_all.at[:, :, columns(owner)], down_all.at[:, :, columns(owner)],
            down_send.at[index], down_recv.at[index], fs, twin,
        )

    down_near.wait_recv()
    echo = hand_down(twin, 2)
    echo.start()
    down_far.wait_recv()
    passed = hand_down(across, 3)
    passed.start()

    lands = side == 1 - (fs // per) % 2

    def hand(a, e):
        return remote(
            full[a].at[e], full[a].at[e], twin_send.at[a, e], twin_recv.at[a, e], fs, twin
        )

    @pl.when(lands)
    def _():
        for a, e in pieces:
            pltpu.make_async_copy(full[a].at[e], full[a].at[e], near_recv.at[a, e]).wait()
            hand(a, e).start()
        for a, e in pieces:
            hand(a, e).wait_send()

    @pl.when(jnp.logical_not(lands))
    def _():
        for a, e in pieces:
            hand(a, e).wait_recv()

    for (a, e), copy in zip(pieces, crossing):
        copy.wait_send()
        pltpu.make_async_copy(own[a].at[e], own[a].at[e], near_send.at[a, e]).wait()
        pltpu.make_async_copy(far[a].at[e], far[a].at[e], far_send.at[a, e]).wait()
    down_near.wait_send()
    down_far.wait_send()
    echo.wait()
    passed.wait()


def apply_experts(x, weight, gate, up, down, gate_out, up_out, down_out, part, total):
    expert, block = pl.program_id(0), pl.program_id(1)
    gate_out[...] = gate[...]
    up_out[...] = up[...]
    down_out[...] = down[...]
    rows = x.shape[0]
    tile = rows // 2

    @pl.when(jnp.logical_and(expert == 0, block == 0))
    def _():
        total[...] = jnp.zeros_like(total)

    def step(i, carry):
        at = pl.ds(pl.multiple_of(i * tile, tile), tile)
        mine = x[at, :]
        gate_val = jnp.dot(mine, gate[0], preferred_element_type=jnp.float32)
        up_val = jnp.dot(mine, up[0], preferred_element_type=jnp.float32)
        hidden = (jax.nn.silu(gate_val) * up_val).astype(jnp.bfloat16)
        result = jnp.dot(hidden, down[0], preferred_element_type=jnp.float32)
        shares = weight[at, :]
        lane = lax.broadcasted_iota(jnp.int32, shares.shape, 1)
        share = jnp.sum(jnp.where(lane == expert, shares, 0.0), axis=1, keepdims=True)
        total[at, :] += share * result
        return carry

    lax.fori_loop(0, rows // tile, step, 0)

    @pl.when(
        jnp.logical_and(expert == pl.num_programs(0) - 1, block == pl.num_programs(1) - 1)
    )
    def _():
        part[...] = total[...].astype(part.dtype)


def fold(chunks, part, out, low_in, mid, high_in, low_send, low_recv, high_send, high_recv):
    highs, _, rows, width = part.shape
    step = width // chunks
    fs, tp = lax.axis_index("fs"), lax.axis_index("tp")
    high, low = fs // 2, fs % 2
    first = []
    for k in range(chunks):
        copy = pltpu.make_async_remote_copy(
            src_ref=part.at[:, 1 - low, :, pl.ds(k * step, step)],
            dst_ref=low_in.at[k],
            send_sem=low_send.at[k],
            recv_sem=low_recv.at[k],
            device_id=(high * 2 + 1 - low, tp),
            device_id_type=MESH,
        )
        copy.start()
        first.append(copy)
    second = []
    for k in range(chunks):
        first[k].wait_recv()
        mid[k] = (
            part[:, low, :, pl.ds(k * step, step)].astype(jnp.float32)
            + low_in[k].astype(jnp.float32)
        ).astype(mid.dtype)
        for shift in range(1, highs):
            to = lax.rem(high + shift, highs)
            copy = pltpu.make_async_remote_copy(
                src_ref=mid.at[k, to],
                dst_ref=high_in.at[k, shift],
                send_sem=high_send.at[k, shift],
                recv_sem=high_recv.at[k, shift],
                device_id=(to * 2 + low, tp),
                device_id_type=MESH,
            )
            copy.start()
            second.append((k, copy))
    for k in range(chunks):
        total = part[high, low, :, pl.ds(k * step, step)].astype(jnp.float32) + low_in[
            k, high
        ].astype(jnp.float32)
        shift = 0
        for at, copy in second:
            if at == k:
                shift += 1
                copy.wait_recv()
                total = total + high_in[k, shift].astype(jnp.float32)
        out[:, pl.ds(k * step, step)] = total.astype(out.dtype)
    for copy in first:
        copy.wait_send()
    for _, copy in second:
        copy.wait_send()


def shards(fs_size, tp_size, tokens, norm_gain, gate_weight, up_weight, down_weight, routes, route_logit):
    experts, depth, width = gate_weight.shape
    _, units, col = down_weight.shape
    rows, features = tokens.shape
    gain_col = norm_gain[None, :, None]
    gate_part = (gate_weight * gain_col).astype(jnp.bfloat16)
    up_part = (up_weight * gain_col).astype(jnp.bfloat16)
    down_part = down_weight.astype(jnp.bfloat16)

    floats = tokens.astype(jnp.float32)
    normed = (floats * lax.rsqrt(jnp.mean(floats * floats, axis=1, keepdims=True) + EPS)).astype(
        jnp.bfloat16
    )
    first_share = jax.nn.sigmoid(route_logit[:, 0] - route_logit[:, 1])
    shares = jnp.stack([first_share, 1.0 - first_share], axis=1)
    named = routes[:, :, None] == jnp.arange(experts, dtype=jnp.int32)[None, None, :]
    weight = jnp.sum(jnp.where(named, shares[:, :, None], 0.0), axis=1)

    half = jnp.bfloat16
    anywhere = pl.BlockSpec(memory_space=pl.ANY)
    dma = pltpu.SemaphoreType.DMA
    gate_shape = jax.ShapeDtypeStruct((experts, features, units), half)
    down_shape = jax.ShapeDtypeStruct((experts, units, features), half)
    far_shape = jax.ShapeDtypeStruct((experts, depth, width), half)
    gate_all, up_all, down_all, _, _ = pl.pallas_call(
        functools.partial(spread, fs_size, tp_size),
        out_shape=(gate_shape, gate_shape, down_shape, far_shape, far_shape),
        in_specs=[anywhere] * 3,
        out_specs=(anywhere,) * 5,
        scratch_shapes=[dma((2, experts))] * 7 + [dma((4,))] * 2,
        compiler_params=pltpu.CompilerParams(has_side_effects=True),
        name="spread",
    )(gate_part, up_part, down_part)

    block = min(units, 512)
    in_wide = pl.BlockSpec((1, features, block), lambda e, j: (e, 0, j))
    in_tall = pl.BlockSpec((1, block, features), lambda e, j: (e, j, 0))
    whole = pl.BlockSpec((rows, features), lambda e, j: (0, 0))
    gate_out, up_out, down_out, part = pl.pallas_call(
        apply_experts,
        grid=(experts, units // block),
        out_shape=(
            gate_shape, gate_shape, down_shape, jax.ShapeDtypeStruct((rows, features), half),
        ),
        in_specs=[
            whole, pl.BlockSpec((rows, experts), lambda e, j: (0, 0)), in_wide, in_wide, in_tall,
        ],
        out_specs=(in_wide, in_wide, in_tall, whole),
        scratch_shapes=[pltpu.VMEM((rows, features), jnp.float32)],
        compiler_params=pltpu.CompilerParams(
            vmem_limit_bytes=VMEM_LIMIT, dimension_semantics=("arbitrary", "arbitrary")
        ),
        name="apply_experts",
    )(normed, weight, gate_all, up_all, down_all)

    highs, mine, chunks = fs_size // 2, rows // fs_size, 4
    step = features // chunks
    vmem = pl.BlockSpec(memory_space=pltpu.VMEM)
    mixed = pl.pallas_call(
        functools.partial(fold, chunks),
        out_shape=jax.ShapeDtypeStruct((mine, features), half),
        in_specs=[vmem],
        out_specs=vmem,
        scratch_shapes=[pltpu.VMEM((chunks, highs, mine, step), half)] * 3
        + [dma((chunks,))] * 2
        + [dma((chunks, highs))] * 2,
        compiler_params=pltpu.CompilerParams(
            has_side_effects=True, vmem_limit_bytes=VMEM_LIMIT // 2
        ),
        name="fold",
    )(part.reshape(highs, 2, mine, features))
    return (gate_out, up_out, down_out, mixed)


def solution(mesh):
    return jax.shard_map(
        functools.partial(shards, mesh.shape["fs"], mesh.shape["tp"]),
        mesh=mesh,
        in_specs=(
            P("tp", None),
            P("fs"),
            P(None, "fs", "tp"),
            P(None, "fs", "tp"),
            P(None, "fs", "tp"),
            P("tp", None),
            P("tp", None),
        ),
        out_specs=(
            P(None, None, "fs"),
            P(None, None, "fs"),
            P(None, "fs", None),
            P(("tp", "fs"), None),
        ),
        check_vma=False,
    )
```
